32 devices in a mesh: ep: 4 (over y, x), tp: 8 (over z, core).
Axes of the slice: x: 2, y: 2, z: 4, core: 2. Of those that a mesh axis runs over, the one named last changes fastest.
Arguments:
- residual: bfloat16 [128, 2048], P('ep'), may hold values from -6 to 6
- mixer_gain: float32 [2048], replicated, may hold values from 0.1 to 1.9
- gate_proj: bfloat16 [2048, 2048], P('ep', 'tp'), may hold values from -0.125 to 0.125
- input_proj: bfloat16 [2048, 2048], P('ep', 'tp'), may hold values from -0.125 to 0.125
- write_proj: bfloat16 [2048, 2048], P('ep', 'tp'), may hold values from -0.125 to 0.125
- read_proj: bfloat16 [2048, 2048], P('ep', 'tp'), may hold values from -0.125 to 0.125
- step_proj: bfloat16 [2048, 32], replicated, may hold values from -0.125 to 0.125
- conv_weight: float32 [4, 3, 2048], replicated, may hold values from -3 to 3
- step_bias: float32 [32], replicated, may hold values from -4 to 0
- log_rate: float32 [32], replicated, may hold values from 0 to 2.5
- skip_gain: float32 [32], replicated, may hold values from -4 to 4
- group_gain: float32 [2048], replicated, may hold values from 0.1 to 1.9
- ssm_state: float32 [128, 32, 64, 128], P('ep', 'tp'), may hold values from -2 to 2
- conv_state: bfloat16 [128, 3, 3, 2048], P('ep', None, None, 'tp'), may hold values from -6 to 6
- out_proj: bfloat16 [2048, 2048], P('tp'), may hold values from -0.125 to 0.125
- ffn_gain: float32 [2048], replicated, may hold values from 0.1 to 1.9
- routes: int32 [128, 2], P('ep'), may hold values from 0 to 7, all different within a row; in each aligned block of 32 rows (0 to 31, 32 to 63, ...) at most 16 rows name the same one
- route_weight: float32 [128, 2], P('ep'), may hold values from 0.2 to 1
- expert_gate: bfloat16 [8, 2048, 2048], P('ep', None, 'tp'), may hold values from -0.125 to 0.125
- expert_up: bfloat16 [8, 2048, 2048], P('ep', None, 'tp'), may hold values from -0.125 to 0.125
- expert_down: bfloat16 [8, 2048, 2048], P('ep', 'tp'), may hold values from -0.125 to 0.125
- dense_gate: bfloat16 [2048, 2048], P(None, 'tp'), may hold values from -0.125 to 0.125
- dense_up: bfloat16 [2048, 2048], P(None, 'tp'), may hold values from -0.125 to 0.125
- dense_down: bfloat16 [2048, 2048], P('tp'), may hold values from -0.125 to 0.125
- blend_weight: bfloat16 [2048], replicated, may hold values from -0.125 to 0.125
Outputs:
- layer_out: bfloat16 [128, 2048], P('ep', 'tp')
- new_state: float32 [128, 32, 64, 128], P('ep', 'tp')
- new_conv: bfloat16 [128, 3, 3, 2048], P('ep', None, None, 'tp')
The draws below stay inside these ranges and needn't reach their ends.
Inputs may be any that keep to these rules, and one draw needn't show every extreme that they name: `routes`: each row names 2 different experts. Within the 32 rows of one index of ep no expert is named by more than 16 rows, and in some such block some expert is named by exactly 16 rows.
All inputs are finite; a program needn't handle non-finite values.
Results may differ from the reference program's by a relative error of at most 0.015.
Values may be sent and summed in bfloat16 or wider, within the bound.
A program may use at most 128 MiB of HBM per device.

```python
import math
import jax
import jax.numpy as jnp
import numpy as np
from jax import lax

D = 2048
HEADS = 32
HEAD_DIM = 64
GROUPS = 16
STATE = 128
KERNEL = 4
TOPK = 2
FFE = 2048
FFD = 2048
S_DEV = 32
D_INNER = 2048
EXPERTS = 8
TOK = 128
CAP = 16
N_EP = 4


def block_levels(stream_key, extent, pieces, smallest, high):
    loudness, own = 1.0, jax.random.fold_in(stream_key, 6)
    for position, shards_of in pieces:
        draws = jnp.exp(jax.random.uniform(jax.random.fold_in(own, position), (shards_of,), jnp.float32, smallest / len(pieces), high / len(pieces)))
        loudness = loudness * jnp.repeat(draws, extent[position] // shards_of).reshape([-1 if axis == position else 1 for axis in range(len(extent))])
    return loudness


def shared_out(key, own, number, rows, number_of, top, reach, lean):
    order = jax.random.permutation(key, number_of)
    heavy_load, ordinary = portions_of(number_of, rows * top, reach, lean, True), portions_of(number_of, rows * top, reach, lean, False)
    places = jnp.arange(number_of)

    def named(sizes, offset_by):
        used = int((sizes > 0).sum())
        fixed = max(1, used // 4)
        moved = fixed + (places - fixed + offset_by * (used - fixed)) % max(1, number_of - fixed)
        return jnp.zeros((number_of,), jnp.int32).at[order[jnp.where(places < fixed, places, moved)]].set(jnp.asarray(sizes, jnp.int32))

    sizes = jnp.where(number % 4 == 0, named(heavy_load, number // 4), named(ordinary, number - number // 4 - 1))
    mixed = jax.random.permutation(jax.random.fold_in(own, 3), number_of)
    giver, sink = mixed[0:number_of // 2 * 2:2], mixed[1:number_of // 2 * 2:2]
    margin = jnp.minimum(sizes[giver] - 1, reach - sizes[sink]) // 2
    margin = jnp.where((giver == order[0]) | (sink == order[0]) | (sizes[sink] == 0), 0, jnp.maximum(margin, 0))
    moved = jax.random.randint(jax.random.fold_in(own, 4), (number_of // 2,), 0, 1 << 20) % (margin + 1)
    sizes = sizes.at[giver].add(-moved).at[sink].add(moved)
    labels = jnp.searchsorted(jnp.cumsum(sizes), jnp.arange(rows * top), side="right").astype(jnp.int32)
    table = labels.reshape(top, rows).T
    table = table[jax.random.permutation(jax.random.fold_in(own, 1), rows)]
    offset_by = jax.random.randint(jax.random.fold_in(own, 2), (rows, 1), 0, top)
    return jnp.take_along_axis(table, (jnp.arange(top)[None, :] + offset_by) % top, axis=1)


def portions_of(amount, total, reach, skew, full):
    loads = [(1 << 20) // math.isqrt(rank ** skew) + 1 for rank in range(1, amount + 1)]
    largest = reach if full else min(reach, max(-(-total // amount), total * loads[0] // sum(loads)))
    least = 1 if total - largest >= amount - 1 else 0
    holding, surplus = [largest] + [least] * (amount - 1), total - largest - least * (amount - 1)
    while surplus > 0:
        candidates = [i for i in range(1, amount) if holding[i] < largest] or [i for i in range(1, amount) if holding[i] < reach]
        whole, left = sum([loads[i] for i in candidates]), surplus
        for i in candidates:
            more = min(reach - holding[i], max(1, left * loads[i] // whole), surplus)
            holding[i] = holding[i] + more
            surplus = surplus - more
    return np.array(holding)


def gaussian(key, dims, deviation, limit, cuts=(), held_as=jnp.bfloat16):
    values = deviation * jax.random.normal(key, dims, jnp.float32)
    if cuts:
        values = values * block_levels(key, dims, cuts, -0.22, 0.18)
    return jnp.clip(values, -limit, limit).astype(held_as)


def setup_inputs(seed: int = 0) -> dict:
    key_list = jax.random.split(jax.random.key(seed), 26)
    residual = gaussian(key_list[0], (TOK, D), 1.0, 6.0, ((0, 4),))
    mixer_gain = jnp.clip(1.0 + 0.18 * jax.random.normal(key_list[1], (D,), jnp.float32), 0.1, 1.9)
    gate_proj = gaussian(key_list[2], (D, D_INNER), D ** -0.5, 0.125, ((0, 4), (1, 8)))
    input_proj = gaussian(key_list[3], (D, D_INNER), D ** -0.5, 0.125, ((0, 4), (1, 8)))
    write_proj = gaussian(key_list[4], (D, D_INNER), D ** -0.5, 0.125, ((0, 4), (1, 8)))
    read_proj = gaussian(key_list[5], (D, D_INNER), D ** -0.5, 0.125, ((0, 4), (1, 8)))
    step_proj = gaussian(key_list[6], (D, HEADS), D ** -0.5, 0.125)
    conv_weight = gaussian(key_list[7], (KERNEL, 3, D_INNER), 0.5, 3.0, (), jnp.float32)
    step_bias = jnp.clip(jax.random.uniform(key_list[8], (HEADS,), jnp.float32, -4.0, 0.0), -4.0, 0.0)
    log_rate = jnp.clip(jax.random.uniform(key_list[9], (HEADS,), jnp.float32, 0.0, 2.5), 0.0, 2.5)
    skip_gain = gaussian(key_list[10], (HEADS,), 1.0, 4.0, (), jnp.float32)
    group_gain = jnp.clip(1.0 + 0.18 * jax.random.normal(key_list[11], (D_INNER,), jnp.float32), 0.1, 1.9)
    ssm_state = gaussian(key_list[12], (TOK, HEADS, HEAD_DIM, STATE), 0.3, 2.0, ((0, 4), (1, 8)), jnp.float32)
    conv_state = gaussian(key_list[13], (TOK, KERNEL - 1, 3, D_INNER), 1.0, 6.0, ((0, 4), (3, 8)))
    out_proj = gaussian(key_list[14], (D_INNER, D), D_INNER ** -0.5, 0.125, ((0, 8),))
    ffn_gain = jnp.clip(1.0 + 0.18 * jax.random.normal(key_list[15], (D,), jnp.float32), 0.1, 1.9)
    routes_keys = jax.random.split(jax.random.fold_in(key_list[16], 1), TOK // S_DEV)
    routes_turns = jax.random.permutation(jax.random.fold_in(key_list[16], 3), TOK // S_DEV)
    routes = jax.vmap(lambda own, number: shared_out(jax.random.fold_in(key_list[16], 2), own, number, S_DEV, EXPERTS, TOPK, CAP, 2))(routes_keys, routes_turns).reshape((TOK, TOPK))
    route_weight = jnp.clip(0.2 + 0.8 * jax.random.uniform(key_list[17], (TOK, TOPK), jnp.float32) ** block_levels(key_list[17], (TOK, TOPK), ((0, 4),), -0.2, 0.2), 0.2, 1.0)
    expert_gate = gaussian(key_list[18], (EXPERTS, D, FFE), D ** -0.5, 0.125, ((0, 4), (2, 8)))
    expert_up = gaussian(key_list[19], (EXPERTS, D, FFE), D ** -0.5, 0.125, ((0, 4), (2, 8)))
    expert_down = gaussian(key_list[20], (EXPERTS, FFE, D), FFE ** -0.5, 0.125, ((0, 4), (1, 8)))
    dense_gate = gaussian(key_list[21], (D, FFD), D ** -0.5, 0.125, ((1, 8),))
    dense_up = gaussian(key_list[22], (D, FFD), D ** -0.5, 0.125, ((1, 8),))
    dense_down = gaussian(key_list[23], (FFD, D), FFD ** -0.5, 0.125, ((0, 8),))
    blend_weight = gaussian(key_list[24], (D,), D ** -0.5, 0.125)
    return {"residual": residual, "mixer_gain": mixer_gain, "gate_proj": gate_proj, "input_proj": input_proj, "write_proj": write_proj, "read_proj": read_proj, "step_proj": step_proj, "conv_weight": conv_weight, "step_bias": step_bias, "log_rate": log_rate, "skip_gain": skip_gain, "group_gain": group_gain, "ssm_state": ssm_state, "conv_state": conv_state, "out_proj": out_proj, "ffn_gain": ffn_gain, "routes": routes, "route_weight": route_weight, "expert_gate": expert_gate, "expert_up": expert_up, "expert_down": expert_down, "dense_gate": dense_gate, "dense_up": dense_up, "dense_down": dense_down, "blend_weight": blend_weight}


epsilon = 1e-06

def rms_rows(values, gain_vector):
    floats_in = values.astype(jnp.float32)
    return floats_in * lax.rsqrt(lax.optimization_barrier(jnp.mean(floats_in * floats_in, axis=-1, keepdims=True)) + epsilon) * gain_vector

def reference(residual, mixer_gain, gate_proj, input_proj, write_proj, read_proj, step_proj, conv_weight, step_bias, log_rate, skip_gain, group_gain, ssm_state, conv_state, out_proj, ffn_gain, routes, route_weight, expert_gate, expert_up, expert_down, dense_gate, dense_up, dense_down, blend_weight):
    normed = rms_rows(residual, mixer_gain).astype(jnp.bfloat16)
    z_proj = jnp.dot(normed, gate_proj, preferred_element_type=jnp.float32).astype(jnp.bfloat16)
    x_proj = jnp.dot(normed, input_proj, preferred_element_type=jnp.float32).astype(jnp.bfloat16)
    b_proj = jnp.dot(normed, write_proj, preferred_element_type=jnp.float32).astype(jnp.bfloat16)
    c_proj = jnp.dot(normed, read_proj, preferred_element_type=jnp.float32).astype(jnp.bfloat16)
    step_raw = jnp.dot(normed, step_proj, preferred_element_type=jnp.float32)
    newest = jnp.stack((x_proj, b_proj, c_proj), axis=1)[:, None]
    stacked = jnp.concatenate((conv_state, newest), axis=1)
    new_conv = stacked[:, 1:]
    activated = jax.nn.silu(jnp.einsum('skcw,kcw->scw', stacked.astype(jnp.float32), conv_weight.astype(jnp.float32)))
    per_group = HEADS // GROUPS
    x_act = activated[:, 0].reshape(TOK, HEADS, HEAD_DIM)
    b_act = jnp.repeat(activated[:, 1].reshape(TOK, GROUPS, STATE), per_group, axis=1)
    c_act = jnp.repeat(activated[:, 2].reshape(TOK, GROUPS, STATE), per_group, axis=1)
    step_size = jax.nn.softplus(step_raw + step_bias)
    decay_factor = jnp.exp(-jnp.exp(log_rate) * step_size)
    new_state = decay_factor[:, :, None, None] * ssm_state + (step_size[:, :, None] * x_act)[..., None] * b_act[:, :, None, :]
    ssm_out = jnp.einsum('shpn,shn->shp', new_state, c_act) + skip_gain[None, :, None] * x_act
    gated_out = ssm_out.reshape(TOK, D_INNER) * jax.nn.silu(z_proj.astype(jnp.float32))
    grouped = gated_out.reshape(TOK, GROUPS, D_INNER // GROUPS)
    grouped = grouped * lax.rsqrt(lax.optimization_barrier(jnp.mean(grouped * grouped, axis=-1, keepdims=True)) + epsilon)
    mixed_out = (grouped.reshape(TOK, D_INNER) * group_gain).astype(jnp.bfloat16)
    resid_mid = (residual.astype(jnp.float32) + jnp.dot(mixed_out, out_proj, preferred_element_type=jnp.float32)).astype(jnp.bfloat16)
    normed_ffn = rms_rows(resid_mid, ffn_gain).astype(jnp.bfloat16)
    flat_routes = routes.reshape(N_EP, S_DEV * TOPK)
    onehot = (flat_routes[..., None] == jnp.arange(EXPERTS, dtype=jnp.int32)).astype(jnp.int32)
    slot_rank = lax.optimization_barrier(jnp.sum((jnp.cumsum(onehot, axis=1) - onehot) * onehot, axis=2)).astype(jnp.int32)
    source = jnp.broadcast_to(jnp.arange(N_EP, dtype=jnp.int32)[:, None], flat_routes.shape)
    repeated = jnp.repeat(normed_ffn, TOPK, axis=0).reshape(N_EP, S_DEV * TOPK, D)
    buffer = jnp.zeros((EXPERTS, N_EP, CAP, D), jnp.bfloat16).at[flat_routes, source, slot_rank].set(repeated)

    def expert(expert_args):
        expert_rows, w_gate, w_up, w_down = expert_args
        expert_rows = expert_rows.reshape(N_EP * CAP, D).astype(jnp.float32)
        gate_val = jnp.dot(expert_rows, w_gate.astype(jnp.float32))
        up_val = jnp.dot(expert_rows, w_up.astype(jnp.float32))
        hidden = (jax.nn.silu(gate_val) * up_val).astype(jnp.bfloat16)
        result = jnp.dot(hidden.astype(jnp.float32), w_down.astype(jnp.float32)).astype(jnp.bfloat16)
        return result.reshape(N_EP, CAP, D)
    results = lax.map(expert, (buffer, expert_gate, expert_up, expert_down))
    picked = results[flat_routes, source, slot_rank].astype(jnp.float32).reshape(TOK, TOPK, D)
    expert_mix = lax.optimization_barrier(jnp.sum(picked * route_weight[..., None], axis=1))
    gate_val = jnp.dot(normed_ffn, dense_gate, preferred_element_type=jnp.float32)
    up_val = jnp.dot(normed_ffn, dense_up, preferred_element_type=jnp.float32)
    dense_hidden = (jax.nn.silu(gate_val) * up_val).astype(jnp.bfloat16)
    dense_out = jnp.dot(dense_hidden, dense_down, preferred_element_type=jnp.float32)
    mix_weight = jax.nn.sigmoid(jnp.dot(normed_ffn, blend_weight, preferred_element_type=jnp.float32))
    layer_out = (resid_mid.astype(jnp.float32) + expert_mix + mix_weight[:, None] * dense_out).astype(jnp.bfloat16)
    return (layer_out, new_state, new_conv)
```

```python
import functools
import jax
import jax.numpy as jnp
from jax import lax
from jax.experimental import pallas as pl
from jax.experimental.pallas import tpu as pltpu
from jax.sharding import PartitionSpec as P

epsilon = 1e-06
F32 = jnp.float32
BF16 = jnp.bfloat16
MESH = pl.DeviceIdType.MESH
VM = pl.BlockSpec(memory_space=pltpu.VMEM)
HB = pl.BlockSpec(memory_space=pltpu.HBM)
GRANT = 50 * 2**20
GRANT2 = 8 * 2**20


def mm(a, b):
    return jnp.dot(a, b, preferred_element_type=F32)


def nt(a, b):
    return lax.dot_general(a, b, (((1,), (1,)), ((), ())), preferred_element_type=F32)


def silu(v):
    return v * jax.nn.sigmoid(v)


def layer_kernel(
    N, T, res_h, mgain_h, wg_h, wx_h, wb_h, wc_h, step_h, bias_h, rate_h, skip_h, ggain_h, taps_h,
    conv_h, st_h, fgain_h, routes_h, rw_h, blend_h, wo_h, eg_h, eu_h, ed_h, dg_h, du_h, dd_h,
    ns_ref, nc_ref, out_ref,
    res, mgain, w, stepw, bias, rate, skip, ggain, taps, conv, st, fgain, routes, rw, blend,
    wo, eg, eu, ed, dg, du, dd,
    nb, pieces, outb1, inb1, s16, dec_rows, act,
    rsb, rsin, ag, nfall, wts, outb, pin, qb, inb, ob, opin, fb, fin_in, own_acc,
    lsem, s1, r1, s2, r2,
    sa, ra, sb, rb, sc, rc, sd, rd, sg, rg, sh, rh, se, re_, so, ro, sf, rf,
):
    ep, tp = lax.axis_index("ep"), lax.axis_index("tp")
    R, D = res.shape
    K = D // N
    W = D // T
    E = eg.shape[0]
    H, PD, S = st.shape[1:]
    G = W // S
    hp = S // PD
    heads = stepw.shape[0]
    kept = conv.shape[0]
    half = R // 2
    core = lax.rem(tp, 2)
    other = 1 - core
    mate = tp + 1 - 2 * core
    own_cols = pl.ds(pl.multiple_of(tp * W, W), W)

    def near(o):
        p, bit = 0, 1
        while bit < N:
            p = p + bit * lax.rem(lax.rem(lax.div(ep, bit), 2) + lax.rem(lax.div(o, bit), 2), 2)
            bit *= 2
        return p

    def tp_copy(src, dst, ss, rs, peer):
        return pltpu.make_async_remote_copy(
            src_ref=src, dst_ref=dst, send_sem=ss, recv_sem=rs,
            device_id=(ep, peer), device_id_type=MESH)

    def ep_copy(src, dst, ss, rs, peer):
        return pltpu.make_async_remote_copy(
            src_ref=src, dst_ref=dst, send_sem=ss, recv_sem=rs,
            device_id=(peer, tp), device_id_type=MESH)

    sources = (
        (res_h, res), (mgain_h, mgain), (wg_h, w.at[0]), (wx_h, w.at[1]), (wb_h, w.at[2]),
        (wc_h, w.at[3]), (step_h, stepw), (bias_h, bias), (rate_h, rate), (skip_h, skip),
        (routes_h, routes), (rw_h, rw), (st_h, st), (conv_h, conv), (taps_h.at[:, :, own_cols], taps),
        (ggain_h.at[:, own_cols], ggain), (wo_h, wo), (fgain_h, fgain), (blend_h, blend),
        (dg_h, dg), (du_h, du), (dd_h, dd), (eg_h, eg), (eu_h, eu), (ed_h, ed),
    )
    loads = [pltpu.make_async_copy(a, b, lsem.at[i]) for i, (a, b) in enumerate(sources)]
    bar = pltpu.get_barrier_semaphore()

    def greet_ep(o, _):
        pl.semaphore_signal(bar, inc=1, device_id=(lax.rem(ep + o, N), tp), device_id_type=MESH)
        return 0

    def greet_tp(o, _):
        pl.semaphore_signal(bar, inc=1, device_id=(ep, lax.rem(tp + o, T)), device_id_type=MESH)
        return 0

    for c in loads[:2]:
        c.start()
    lax.fori_loop(1, N, greet_ep, 0)
    lax.fori_loop(1, T, greet_tp, 0)
    for c in loads[2:12]:
        c.start()
    for c in loads[:2]:
        c.wait()
    x = res[...].astype(F32)
    normed = x * lax.rsqrt(jnp.mean(x * x, axis=-1, keepdims=True) + epsilon) * mgain[...]
    normed = normed.astype(BF16)
    for k in range(N):
        nb[k] = normed[:, k * K:(k + 1) * K]
    pl.semaphore_wait(bar, N - 1 + T - 1)

    def send1(o, _):
        p = near(o)
        ep_copy(nb.at[p], pieces.at[ep], s1.at[p], r1.at[ep], p).start()
        return 0

    lax.fori_loop(1, N, send1, 0)
    for c in loads[12:17]:
        c.start()
    for c in loads[6:12]:
        c.wait()

    raw = nt(normed, stepw[...])
    size = jax.nn.softplus(raw + bias[...])
    decay = jnp.exp(-jnp.exp(rate[...]) * size)
    table = jnp.concatenate((size, decay, jnp.broadcast_to(skip[...], (8, heads))), axis=0)
    row = lax.broadcasted_iota(jnp.int32, (heads, W), 0)
    col = lax.broadcasted_iota(jnp.int32, (heads, W), 1)
    pick = (row == tp * H + col // PD).astype(F32)
    wide = jnp.dot(table, pick, preferred_element_type=F32, precision=lax.Precision.HIGHEST)
    row = lax.broadcasted_iota(jnp.int32, (heads, H * S), 0)
    col = lax.broadcasted_iota(jnp.int32, (heads, H * S), 1)
    pick = (row == tp * H + col // S).astype(F32)
    dec_rows[...] = jnp.dot(decay, pick, preferred_element_type=F32, precision=lax.Precision.HIGHEST)

    L = wts.shape[2]
    line = lax.broadcasted_iota(jnp.int32, (L, R), 0)
    table = jnp.zeros((L, R), F32)
    for k in range(routes.shape[0]):
        table = table + jnp.where(line == routes[k:k + 1, :], rw[k:k + 1, :], 0.0)
    eye = (lax.broadcasted_iota(jnp.int32, (L, L), 0) == lax.broadcasted_iota(jnp.int32, (L, L), 1))
    wts[ep] = lax.dot_general(
        table, eye.astype(F32), (((0,), (0,)), ((), ())), preferred_element_type=F32,
        precision=lax.Precision.HIGHEST)

    for c in loads[2:6]:
        c.wait()
    own = [mm(nb[ep], w[i]) for i in range(4)]

    def step(o, _):
        p = near(o)
        ep_copy(nb.at[p], pieces.at[p], s1.at[p], r1.at[p], p).wait_recv()
        a = pieces[p]
        for i in range(4):
            outb1[p, :, i * W:(i + 1) * W] = mm(a, w[i]).astype(BF16)
        ep_copy(outb1.at[p], inb1.at[ep], s2.at[p], r2.at[ep], p).start()
        return 0

    lax.fori_loop(1, N, step, 0)

    def send_w(o, _):
        p = near(o)
        ep_copy(wts.at[ep], wts.at[ep], sb.at[p], rb.at[ep], p).start()
        return 0

    lax.fori_loop(1, N, send_w, 0)
    for c in loads[17:]:
        c.start()
    for c in loads[12:16]:
        c.wait()

    def narrow(i, _):
        for j in range(4):
            s = i * 4 + j
            for g in range(G):
                s16[s, :, g * S:(g + 1) * S] = st[s, g * hp:(g + 1) * hp].reshape(S, S).astype(BF16)
        return 0

    lax.fori_loop(0, R // 4, narrow, 0)
    for c in range(3):
        part = jnp.zeros((R, W), F32)
        for k in range(kept):
            part = part + conv[k, c].astype(F32) * taps[c, k:k + 1, :]
        act[c] = part
        for k in range(kept - 1):
            nc_ref[k, c] = conv[k + 1, c]

    total = jnp.concatenate(own, axis=1)
    for o in range(1, N):
        p = near(o)
        ep_copy(outb1.at[p], inb1.at[p], s2.at[p], r2.at[p], p).wait_recv()
        total = total + inb1[p].astype(F32)
    proj = total.astype(BF16)
    channels = []
    for c in range(3):
        newest = proj[:, (c + 1) * W:(c + 2) * W]
        nc_ref[kept - 1, c] = newest
        channels.append(silu(act[c] + newest.astype(F32) * taps[c, kept:kept + 1, :]))
    xa, bm, cm = channels
    sx = wide[:R] * xa
    act[0] = sx
    act[1] = bm
    lane = lax.broadcasted_iota(jnp.int32, (8, W), 1) // S
    line = lax.broadcasted_iota(jnp.int32, (8, S), 0)
    rows_out = []
    for blk in range(R // 8):
        c8 = cm[blk * 8:(blk + 1) * 8]
        lhs = jnp.concatenate([jnp.where(lane == g, c8, 0.0) for g in range(G)], axis=0).astype(BF16)
        ys = [jnp.zeros((8, S), F32) for _ in range(G)]
        for j in range(0, 8, 2):
            s = blk * 8 + j
            got = nt(lhs, s16[s:s + 2].reshape(2 * S, W))
            for g in range(G):
                for i in range(2):
                    ys[g] = jnp.where(line == j + i, got[g * 8:(g + 1) * 8, i * S:(i + 1) * S], ys[g])
        rows_out.append(jnp.concatenate(ys, axis=1))
    y = wide[R:2 * R] * jnp.concatenate(rows_out, axis=0)
    bc = bm * cm
    z = silu(proj[:, :W].astype(F32))
    direct = wide[2 * R:2 * R + 1] * xa
    mixed = []
    for g in range(G):
        cols = slice(g * S, (g + 1) * S)
        dots = jnp.sum(bc[:, cols], axis=-1, keepdims=True)
        v = (y[:, cols] + dots * sx[:, cols] + direct[:, cols]) * z[:, cols]
        v = v * lax.rsqrt(jnp.mean(v * v, axis=-1, keepdims=True) + epsilon)
        mixed.append((v * ggain[:, cols]).astype(BF16))
    mixed = jnp.concatenate(mixed, axis=1)
    loads[16].wait()
    for k in range(T):
        rsb[k] = mm(mixed, wo[:, k * W:(k + 1) * W]).astype(BF16)

    def send_a(o, _):
        p = lax.rem(tp + o, T)
        tp_copy(rsb.at[p], rsin.at[tp], sa.at[p], ra.at[tp], p).start()
        return 0

    lax.fori_loop(1, T, send_a, 0)

    def update(i, _):
        here = pl.ds(pl.multiple_of(i * 8, 8), 8)
        sx8, b8, dec = act[0, here, :], act[1, here, :], dec_rows[here, :]
        sxT = jnp.concatenate((sx8, jnp.zeros((S - 8, W), F32)), axis=0).T
        for g in range(G):
            for j in range(8):
                bg = b8[j:j + 1, g * S:(g + 1) * S]
                for h in range(g * hp, (g + 1) * hp):
                    column = sxT[h * PD:(h + 1) * PD, j:j + 1]
                    ns_ref[i * 8 + j, h] = dec[j:j + 1, h * S:(h + 1) * S] * st[i * 8 + j, h] + column * bg
        return 0

    lax.fori_loop(0, R // 8, update, 0)

    def sum_a(o, acc):
        p = lax.rem(tp + o, T)
        tp_copy(rsb.at[p], rsin.at[p], sa.at[p], ra.at[p], p).wait_recv()
        return acc + rsin[p].astype(F32)

    total = lax.fori_loop(1, T, sum_a, rsb[tp].astype(F32))
    ag[tp] = (res[:, own_cols].astype(F32) + total).astype(BF16)

    def send_c(o, _):
        p = lax.rem(tp + o, T)
        tp_copy(ag.at[tp], ag.at[tp], sc.at[p], rc.at[tp], p).start()
        return 0

    lax.fori_loop(1, T, send_c, 0)

    def wait_c(o, _):
        p = lax.rem(tp + o, T)
        tp_copy(ag.at[p], ag.at[p], sc.at[p], rc.at[p], p).wait_recv()
        return 0

    lax.fori_loop(1, T, wait_c, 0)
    loads[17].wait()
    sq = jnp.zeros((R, 1), F32)
    for k in range(T):
        v = ag[k].astype(F32)
        sq = sq + jnp.sum(v * v, axis=-1, keepdims=True)
    scale = lax.rsqrt(sq / D + epsilon)
    for k in range(T):
        cols = slice(k * W, (k + 1) * W)
        v = (ag[k].astype(F32) * scale * fgain[:, cols]).astype(BF16)
        nfall[ep, 0, :, cols] = v[:half]
        nfall[ep, 1, :, cols] = v[half:]

    def send_d(o, _):
        p = near(o)
        ep_copy(nfall.at[ep, core], nfall.at[ep, core], sd.at[p], rd.at[ep], p).start()
        return 0

    lax.fori_loop(1, N, send_d, 0)

    nf = nfall[ep].reshape(R, D)
    for c in loads[18:22]:
        c.wait()
    dh = (silu(mm(nf, dg[...])) * mm(nf, du[...])).astype(BF16)
    blend = jnp.sum(nf.astype(F32) * blend[...].astype(F32).reshape(1, D), axis=-1, keepdims=True)
    mixw = jax.nn.sigmoid(blend)
    own = mm(dh, dd[...]) * mixw
    for c in loads[22:]:
        c.wait()

    elane = lax.broadcasted_iota(jnp.int32, (R, wts.shape[2]), 1)

    def experts(p):
        rows = nfall[p].reshape(R, D)
        table = wts[p]
        acc = None
        for e in range(E):
            coef = jnp.sum(jnp.where(elane == ep * E + e, table, 0.0), axis=-1, keepdims=True)
            h = (silu(mm(rows, eg[e])) * mm(rows, eu[e])).astype(BF16)
            part = mm(h, ed[e]) * coef
            acc = part if acc is None else acc + part
        return acc

    own_acc[...] = (own + experts(ep)).reshape(2, half, D)
    ob[...] = own_acc[other].astype(BF16)
    own_swap = tp_copy(ob, opin, so.at[0], ro.at[0], mate)
    own_swap.start()

    def forward(o, _):
        p = near(o)
        ep_copy(nfall.at[p, core], nfall.at[p, core], sd.at[p], rd.at[p], p).wait_recv()
        tp_copy(nfall.at[p, core], nfall.at[p, core], sg.at[p], rg.at[p], mate).start()
        return 0

    lax.fori_loop(1, N, forward, 0)

    def hand_back(o):
        p = near(o)
        tp_copy(outb.at[p, other], pin.at[p], sh.at[p], rh.at[p], mate).wait_recv()
        qb[p] = (outb[p, core].astype(F32) + pin[p].astype(F32)).astype(BF16)
        ep_copy(qb.at[p], inb.at[ep], se.at[p], re_.at[ep], p).start()

    def visit(o, _):
        p = near(o)
        ep_copy(wts.at[p], wts.at[p], sb.at[p], rb.at[p], p).wait_recv()
        tp_copy(nfall.at[p, other], nfall.at[p, other], sg.at[p], rg.at[p], mate).wait_recv()
        outb[p] = experts(p).astype(BF16).reshape(2, half, D)
        tp_copy(outb.at[p, other], pin.at[p], sh.at[p], rh.at[p], mate).start()

        @pl.when(o > 1)
        def _():
            hand_back(o - 1)

        return 0

    lax.fori_loop(1, N, visit, 0)
    hand_back(jnp.int32(N - 1))
    own_swap.wait()
    own_acc[core] += opin[...].astype(F32)

    def gather_e(o, _):
        p = near(o)
        ep_copy(qb.at[p], inb.at[p], se.at[p], re_.at[p], p).wait_recv()
        own_acc[core] += inb[p].astype(F32)
        return 0

    lax.fori_loop(1, N, gather_e, 0)
    for k in range(T):
        fb[k] = own_acc[core, :, k * W:(k + 1) * W].astype(BF16)

    def send_f(o, _):
        p = lax.rem(tp + o, T)
        tp_copy(fb.at[p], fin_in.at[tp], sf.at[p], rf.at[tp], p).start()
        return 0

    lax.fori_loop(1, T, send_f, 0)
    fin_in[tp] = fb[tp]

    def wait_f(o, _):
        p = lax.rem(tp + o, T)
        tp_copy(fb.at[p], fin_in.at[p], sf.at[p], rf.at[p], p).wait_recv()
        return 0

    lax.fori_loop(1, T, wait_f, 0)
    halves = [sum(fin_in[k].astype(F32) for k in range(i, T, 2)) for i in range(2)]
    final = jnp.concatenate(halves, axis=0) + ag[tp].astype(F32)
    out_ref[...] = final.astype(BF16)

    def done_tp(o, _):
        p = lax.rem(tp + o, T)
        tp_copy(rsb.at[p], rsin.at[p], sa.at[p], ra.at[p], p).wait_send()
        tp_copy(ag.at[tp], ag.at[tp], sc.at[p], rc.at[p], p).wait_send()
        tp_copy(fb.at[p], fin_in.at[p], sf.at[p], rf.at[p], p).wait_send()
        return 0

    def done_ep(o, _):
        p = near(o)
        ep_copy(nb.at[p], pieces.at[p], s1.at[p], r1.at[p], p).wait_send()
        ep_copy(outb1.at[p], inb1.at[p], s2.at[p], r2.at[p], p).wait_send()
        ep_copy(wts.at[ep], wts.at[ep], sb.at[p], rb.at[p], p).wait_send()
        ep_copy(nfall.at[ep, core], nfall.at[ep, core], sd.at[p], rd.at[p], p).wait_send()
        tp_copy(nfall.at[p, core], nfall.at[p, core], sg.at[p], rg.at[p], mate).wait_send()
        tp_copy(outb.at[p, other], pin.at[p], sh.at[p], rh.at[p], mate).wait_send()
        ep_copy(qb.at[p], inb.at[p], se.at[p], re_.at[p], p).wait_send()
        return 0

    lax.fori_loop(1, T, done_tp, 0)
    lax.fori_loop(1, N, done_ep, 0)


def write_kernel(ns, nc, out, ns_h, nc_h, out_h, sem):
    n = sem.shape[0] - 2
    rows = ns.shape[0] // n
    copies = [
        pltpu.make_async_copy(ns.at[pl.ds(i * rows, rows)], ns_h.at[pl.ds(i * rows, rows)], sem.at[i])
        for i in range(n)
    ]
    copies.append(pltpu.make_async_copy(nc, nc_h, sem.at[n]))
    copies.append(pltpu.make_async_copy(out, out_h, sem.at[n + 1]))
    for c in copies:
        c.start()
    for c in copies:
        c.wait()


def on_device(
    residual, mixer_gain, gate_proj, input_proj, write_proj, read_proj, step_proj, conv_weight,
    step_bias, log_rate, skip_gain, group_gain, ssm_state, conv_state, out_proj, ffn_gain, routes,
    route_weight, expert_gate, expert_up, expert_down, dense_gate, dense_up, dense_down,
    blend_weight,
):
    N, T = lax.axis_size("ep"), lax.axis_size("tp")
    R, D = residual.shape
    K, W = gate_proj.shape
    H, PD, S = ssm_state.shape[1:]
    E = expert_gate.shape[0]
    heads = step_proj.shape[1]
    kept = conv_state.shape[1]
    top = routes.shape[1]
    G = W // S
    dma = pltpu.SemaphoreType.DMA
    V = pltpu.VMEM
    lanes = max(128, -(-E * N // 128) * 128)
    n_in = 25
    new_state, conv_out, last = pl.pallas_call(
        functools.partial(layer_kernel, N, T),
        out_shape=(V(ssm_state.shape, F32), V((kept, 3, R, W), BF16), V((R, W), BF16)),
        in_specs=[HB] * n_in,
        out_specs=(VM, VM, VM),
        scratch_shapes=[
            V((R, D), BF16), V((1, D), F32), V((4, K, W), BF16), V((heads, D), BF16),
            V((1, heads), F32), V((1, heads), F32), V((1, heads), F32), V((1, W), F32),
            V((3, kept + 1, W), F32), V((kept, 3, R, W), BF16), V(ssm_state.shape, F32),
            V((1, D), F32), V((top, R), jnp.int32), V((top, R), F32), V((D,), BF16),
            V((W, D), BF16), V((E, D, W), BF16), V((E, D, W), BF16), V((E, W, D), BF16),
            V((D, W), BF16), V((D, W), BF16), V((W, D), BF16),
            V((N, R, K), BF16), V((N, R, K), BF16), V((N, R, 4 * W), BF16), V((N, R, 4 * W), BF16),
            V((R, S, W), BF16), V((R, H * S), F32), V((3, R, W), F32),
            V((T, R, W), BF16), V((T, R, W), BF16), V((T, R, W), BF16),
            V((N, 2, R // 2, D), BF16), V((N, R, lanes), F32),
            V((N, 2, R // 2, D), BF16), V((N, R // 2, D), BF16),
            V((N, R // 2, D), BF16), V((N, R // 2, D), BF16),
            V((R // 2, D), BF16), V((R // 2, D), BF16),
            V((T, R // 2, W), BF16), V((T, R // 2, W), BF16),
            V((2, R // 2, D), F32),
            dma((n_in,)), dma((N,)), dma((N,)), dma((N,)), dma((N,)),
            dma((T,)), dma((T,)), dma((N,)), dma((N,)), dma((T,)), dma((T,)),
            dma((N,)), dma((N,)), dma((N,)), dma((N,)), dma((N,)), dma((N,)), dma((N,)), dma((N,)),
            dma((1,)), dma((1,)), dma((T,)), dma((T,)),
        ],
        compiler_params=pltpu.CompilerParams(
            collective_id=0, has_side_effects=True, vmem_limit_bytes=GRANT),
        name="layer",
    )(residual, mixer_gain.reshape(1, D), gate_proj, input_proj, write_proj, read_proj, step_proj.T,
      step_bias.reshape(1, heads), log_rate.reshape(1, heads), skip_gain.reshape(1, heads),
      group_gain.reshape(1, D), conv_weight.transpose(1, 0, 2), conv_state.transpose(1, 2, 0, 3),
      ssm_state, ffn_gain.reshape(1, D), routes.T, route_weight.T, blend_weight,
      out_proj, expert_gate, expert_up, expert_down, dense_gate, dense_up, dense_down)
    new_state, conv_out, layer_out = pl.pallas_call(
        write_kernel,
        out_shape=(
            jax.ShapeDtypeStruct(ssm_state.shape, F32),
            jax.ShapeDtypeStruct((kept, 3, R, W), BF16),
            jax.ShapeDtypeStruct((R, W), BF16),
        ),
        in_specs=[VM] * 3,
        out_specs=(HB, HB, HB),
        scratch_shapes=[dma((10,))],
        compiler_params=pltpu.CompilerParams(vmem_limit_bytes=GRANT2),
        name="write",
    )(new_state, conv_out, last)
    return (layer_out, new_state, conv_out.transpose(2, 0, 1, 3))


def solution(mesh):
    return jax.shard_map(
        on_device,
        mesh=mesh,
        in_specs=(
            P("ep", None), P(), P("ep", "tp"), P("ep", "tp"), P("ep", "tp"), P("ep", "tp"),
            P(), P(), P(), P(), P(), P(),
            P("ep", "tp", None, None), P("ep", None, None, "tp"), P("tp", None), P(),
            P("ep", None), P("ep", None), P("ep", None, "tp"), P("ep", None, "tp"),
            P("ep", "tp", None), P(None, "tp"), P(None, "tp"), P("tp", None), P(),
        ),
        out_specs=(P("ep", "tp"), P("ep", "tp", None, None), P("ep", None, None, "tp")),
        check_vma=False,
    )
```
